32 devices in a mesh: sp: 8 (over z, y), tp: 4 (over x, core).
Axes of the slice: x: 2, y: 2, z: 4, core: 2. Of those that a mesh axis runs over, the one named last changes fastest.
Arguments:
- tokens: bfloat16 [1536, 2048], P(('sp', 'tp')), may hold values from -6 to 6
- norm_in: float32 [2048], replicated, may hold values from 0.1 to 1.9
- decay_log: float32 [128, 64], P('tp'), may hold values from -0.034 to -0.00016276042, as said below
- phase: float32 [128, 64], P('tp'), may hold values from -1 to 1
- b_real: float32 [128, 64, 16], P('tp'), may hold values from -1 to 1
- b_imag: float32 [128, 64, 16], P('tp'), may hold values from -1 to 1
- c_real: float32 [128, 16, 64], P('tp'), may hold values from -0.75 to 0.75
- c_imag: float32 [128, 16, 64], P('tp'), may hold values from -0.75 to 0.75
- skip_gain: float32 [2048], P('tp'), may hold values from -6 to 6
- w_value: bfloat16 [2048, 2048], P(None, 'tp'), as said below
- w_gate: bfloat16 [2048, 2048], P(None, 'tp'), may hold values from -0.125 to 0.125
- norm_out: float32 [2048], P('tp'), may hold values from 0.1 to 1.9
Outputs:
- mixed: bfloat16 [1536, 2048], P('sp', 'tp')
The draws below stay inside these ranges and needn't reach their ends.
Inputs may be any that keep to these rules, and one draw needn't show every extreme that they name: `decay_log`: negative real parts of the eigenvalues. `w_value`: weights of the value projection.
All inputs are finite; a program needn't handle non-finite values.
Results may differ from the reference program's by a relative error of at most 0.012.
The reference program's roundings to bfloat16 on the way count: a program that leaves them out, or rounds other values in their place, can miss the bound.
Values may be sent and summed in bfloat16 or wider, within the bound.
A program may use at most 64 MiB of HBM per device.

```python
import math
import jax
import jax.numpy as jnp
from jax import lax

D = 2048
GROUP = 16
STATE = 64
GROUPS = 128
TOK_DEV = 192
TOKENS = 1536
N_SP = 8


def draw_decay_log(key, part):
    first_key = jax.random.fold_in(key, 11)
    second_key = jax.random.fold_in(key, 12)
    third_key = jax.random.fold_in(key, 13)
    slow_share = 0.5
    slow_flag = jax.random.uniform(first_key, (GROUPS, 1), jnp.float32) < slow_share
    slow_rate = jnp.exp(jax.random.uniform(second_key, (GROUPS, STATE), jnp.float32, math.log(0.25), math.log(2.2))) / TOKENS
    fast_rate = jnp.exp(jax.random.uniform(third_key, (GROUPS, STATE), jnp.float32, math.log(0.0101), math.log(0.0333)))
    return -jnp.where(slow_flag, slow_rate, fast_rate)


def draw_w_value(key, part):
    top_scale = 10.0
    columns = jnp.arange(D, dtype=jnp.float32)
    column_scale = jnp.exp(math.log(top_scale) * columns / D)
    base = jax.random.normal(key, (D, D), jnp.float32) * D ** (-0.5)
    return (base * column_scale[None, :]).astype(jnp.bfloat16)


def block_levels(key, dims, shards, low, top_value):
    def one(dim, shards_of):
        steps = jax.random.uniform(jax.random.fold_in(jax.random.fold_in(key, 6), dim), (shards_of,), jnp.float32, low / len(shards), top_value / len(shards))
        return jnp.repeat(jnp.exp(steps), dims[dim] // shards_of).reshape((-1,) + (1,) * (len(dims) - dim - 1))

    level = one(*shards[0])
    for cut in shards[1:]:
        level = level * one(*cut)
    return level


def centred(rng, dims, spread, bound, cuts=(), kind=jnp.bfloat16):
    result = jax.random.normal(rng, dims, jnp.float32) * spread
    if len(cuts) > 0:
        result = block_levels(rng, dims, cuts, -0.22, 0.18) * result
    return jnp.clip(result, min=-bound, max=bound).astype(kind)


def setup_inputs(seed: int = 0) -> dict:
    splits = jax.random.split(jax.random.key(seed), 13)
    return {
        "tokens": centred(splits[0], (TOKENS, D), 1.0, 6.0, ((0, 32),)),
        "norm_in": jnp.clip(1.0 + 0.18 * jax.random.normal(splits[1], (D,), jnp.float32), 0.1, 1.9),
        "decay_log": draw_decay_log(jax.random.fold_in(splits[12], 71), 0),
        "phase": jnp.clip(jax.random.uniform(splits[3], (GROUPS, STATE), jnp.float32, -1.0, 1.0) * block_levels(splits[3], (GROUPS, STATE), ((0, 4),), -0.4, 0.0), -1.0, 1.0),
        "b_real": centred(splits[4], (GROUPS, STATE, GROUP), (2 * GROUP) ** -0.5, 1.0, ((0, 4),), jnp.float32),
        "b_imag": centred(splits[5], (GROUPS, STATE, GROUP), (2 * GROUP) ** -0.5, 1.0, ((0, 4),), jnp.float32),
        "c_real": centred(splits[6], (GROUPS, GROUP, STATE), STATE ** -0.5, 0.75, ((0, 4),), jnp.float32),
        "c_imag": centred(splits[7], (GROUPS, GROUP, STATE), STATE ** -0.5, 0.75, ((0, 4),), jnp.float32),
        "skip_gain": centred(splits[8], (D,), 1.0, 6.0, ((0, 4),), jnp.float32),
        "w_value": draw_w_value(jax.random.fold_in(splits[12], 71), 0),
        "w_gate": centred(splits[10], (D, D), D ** -0.5, 0.125, ((1, 4),)),
        "norm_out": jnp.clip(1.0 + 0.18 * jax.random.normal(splits[11], (D,), jnp.float32), 0.1, 1.9),
    }


NORM_EPS = 1e-06
HIGHEST_PREC = lax.Precision.HIGHEST

def coefficients(decay_log, phase, b_real, b_imag):
    magnitude = jnp.exp(decay_log)
    bar_re = magnitude * jnp.cos(phase)
    bar_im = magnitude * jnp.sin(phase)
    modulus = decay_log * decay_log + phase * phase
    coef_re = ((bar_re - 1.0) * decay_log + bar_im * phase) / modulus
    coef_im = (bar_im * decay_log - (bar_re - 1.0) * phase) / modulus
    in_re = coef_re[:, :, None] * b_real - coef_im[:, :, None] * b_imag
    in_im = coef_re[:, :, None] * b_imag + coef_im[:, :, None] * b_real
    return (bar_re, bar_im, in_re, in_im)

def prefix_states(drive_re, drive_im, rate_re, rate_im):
    length = drive_re.shape[0]
    stride = 1
    for level in range(max(length - 1, 1).bit_length()):
        padding = jnp.zeros((stride,) + drive_re.shape[1:], jnp.float32)
        moved_re = jnp.concatenate([padding, drive_re[:length - stride]], axis=0)
        moved_im = jnp.concatenate([padding, drive_im[:length - stride]], axis=0)
        drive_re, drive_im = (drive_re + rate_re * moved_re - rate_im * moved_im, drive_im + rate_re * moved_im + rate_im * moved_re)
        rate_re, rate_im = (rate_re * rate_re - rate_im * rate_im, 2.0 * rate_re * rate_im)
        stride = stride * 2
    return (drive_re, drive_im)

def readout(state_re, state_im, c_real, c_imag):
    first = jnp.einsum('tgp,ghp->tgh', state_re, c_real, precision=HIGHEST_PREC)
    second = jnp.einsum('tgp,ghp->tgh', state_im, c_imag, precision=HIGHEST_PREC)
    return first - second

def reference(tokens, norm_in, decay_log, phase, b_real, b_imag, c_real, c_imag, skip_gain, w_value, w_gate, norm_out):
    xf = tokens.astype(jnp.float32)
    normed = (xf * lax.rsqrt(lax.optimization_barrier(jnp.mean(xf * xf, axis=1, keepdims=True)) + NORM_EPS) * norm_in).astype(jnp.bfloat16)
    bar_re, bar_im, bb_re, bb_im = coefficients(decay_log, phase, b_real, b_imag)
    blocks = normed.reshape(N_SP, TOK_DEV, GROUPS, GROUP)
    skip_grid = skip_gain.reshape(GROUPS, GROUP)

    def block_step(carried, block):
        state_re, state_im = carried
        drive = block.astype(jnp.float32)
        in_re = jnp.einsum('tgh,gph->tgp', drive, bb_re, precision=HIGHEST_PREC)
        in_im = jnp.einsum('tgh,gph->tgp', drive, bb_im, precision=HIGHEST_PREC)
        in_re = in_re.at[0].add(bar_re * state_re - bar_im * state_im)
        in_im = in_im.at[0].add(bar_re * state_im + bar_im * state_re)
        all_re, all_im = prefix_states(in_re, in_im, bar_re, bar_im)
        mixed_pre = readout(all_re, all_im, c_real, c_imag) + skip_grid * drive
        z_block = jax.nn.gelu(mixed_pre).reshape(TOK_DEV, D).astype(jnp.bfloat16)
        return ((all_re[-1], all_im[-1]), z_block)
    start_state = (jnp.zeros((GROUPS, STATE), jnp.float32), jnp.zeros((GROUPS, STATE), jnp.float32))
    ignored, z_blocks = lax.scan(block_step, start_state, blocks)
    z_all = z_blocks.reshape(N_SP * TOK_DEV, D)
    projected_value = jnp.dot(z_all, w_value, preferred_element_type=jnp.float32)
    projected_gate = jnp.dot(z_all, w_gate, preferred_element_type=jnp.float32)
    gated = projected_value * jax.nn.sigmoid(projected_gate)
    scale = lax.rsqrt(lax.optimization_barrier(jnp.mean(gated * gated, axis=1, keepdims=True)) + NORM_EPS)
    return (gated * scale * norm_out).astype(jnp.bfloat16)
```

```python
import functools

import jax
import jax.numpy as jnp
from jax import lax
from jax.experimental import pallas as pl
from jax.experimental.pallas import tpu as pltpu
from jax.sharding import PartitionSpec as P

NORM_EPS = 1e-06
LANES = 128
F32 = jnp.float32
BF16 = jnp.bfloat16
HIGHEST = lax.Precision.HIGHEST
NT = (((1,), (1,)), ((), ()))


def cmul(ar, ai, br, bi):
    return ar * br - ai * bi, ar * bi + ai * br


def remote(src, dst, send, recv, target):
    return pltpu.make_async_remote_copy(
        src_ref=src,
        dst_ref=dst,
        send_sem=send,
        recv_sem=recv,
        device_id=target,
        device_id_type=pl.DeviceIdType.MESH,
    )


def layer(
    n_sp, n_tp, state, group,
    tok, nin, dlog, phase, bre_h, bim_h, cre_h, cim_h, skip, wv_h, wg_h, nout,
    out,
    nsend, urecv, uf, ub, rows_a, rows_p, t1r, t1i, t2r, t2i, bs, cs, wbuf, ylocal,
    e_f, e_send, e_all, l_ref, zbuf, wv, wg, acc_v, acc_g, sq_all,
    bre, bim, cre, cim,
    load_sem, a_send, a_recv, e_ssem, e_rsem, z_send, z_recv, f_send, q_send, q_recv,
):
    sp, tp = lax.axis_index("sp"), lax.axis_index("tp")
    mine, d_model = tok.shape
    rows, width = uf.shape
    n_blk = width // LANES
    per = LANES // group
    lanes = per * state
    core = lax.rem(tp, 2)
    partner = tp + 1 - 2 * core
    n_chip = n_tp // 2

    barrier = pltpu.get_barrier_semaphore()
    for k in range(1, n_tp):
        pl.semaphore_signal(
            barrier, inc=1, device_id={"tp": lax.rem(tp + k, n_tp)},
            device_id_type=pl.DeviceIdType.MESH,
        )

    def greet(k, c):
        pl.semaphore_signal(
            barrier, inc=1, device_id={"sp": lax.rem(sp + k, n_sp)},
            device_id_type=pl.DeviceIdType.MESH,
        )
        return c

    lax.fori_loop(1, n_sp, greet, 0)

    loads = [
        pltpu.make_async_copy(src, dst, load_sem.at[i])
        for i, (src, dst) in enumerate(
            ((bre_h, bre), (bim_h, bim), (cre_h, cre), (cim_h, cim), (wv_h, wv), (wg_h, wg))
        )
    ]
    for copy in loads:
        copy.start()

    xf = tok[...].astype(F32)
    scale = lax.rsqrt(jnp.sum(xf * xf, axis=1, keepdims=True) / d_model + NORM_EPS)
    normed = (xf * scale * nin[...]).astype(BF16)
    for j in range(n_tp):
        nsend[j] = normed[:, j * width : (j + 1) * width]

    side = LANES // state
    for i in range(width // group // side):
        cut = slice(i * LANES, (i + 1) * LANES)
        for src, dst in ((dlog, rows_a), (phase, rows_p)):
            row = jnp.concatenate([src[i * side + k : i * side + k + 1, :] for k in range(side)], axis=1)
            dst[:, cut] = jnp.broadcast_to(row, (8, LANES))

    pl.semaphore_wait(barrier, n_tp - 1 + n_sp - 1)

    sends = []
    for k in range(1, n_tp):
        j = lax.rem(tp + n_tp - k, n_tp)
        copy = remote(nsend.at[j], urecv.at[tp], a_send.at[k], a_recv.at[tp], {"tp": j})
        copy.start()
        sends.append(copy)
    urecv[tp] = nsend[tp]

    for blk in range(n_blk):
        cut = slice(blk * lanes, (blk + 1) * lanes)
        a, p = rows_a[:, cut], rows_p[:, cut]
        k = lax.broadcasted_iota(jnp.int32, a.shape, 0).astype(F32)
        mag, cos, sin = jnp.exp(a), jnp.cos(p), jnp.sin(p)
        lr, li = mag * cos, mag * sin
        inv = jnp.exp(-a)
        nr, ni = inv * cos, -inv * sin
        mod = a * a + p * p
        cr = ((lr - 1.0) * a + li * p) / mod
        ci = (li * a - (lr - 1.0) * p) / mod
        one, zero = jnp.ones_like(a), jnp.zeros_like(a)
        pr, pi, mr, mi = one, zero, cr, ci
        sr, si, qr, qi = lr, li, nr, ni
        row = lax.broadcasted_iota(jnp.int32, a.shape, 0)
        for bit in range(3):
            on = lax.rem(row // (1 << bit), 2) == 1
            ar, ai = cmul(pr, pi, sr, si)
            pr, pi = jnp.where(on, ar, pr), jnp.where(on, ai, pi)
            ar, ai = cmul(mr, mi, qr, qi)
            mr, mi = jnp.where(on, ar, mr), jnp.where(on, ai, mi)
            sr, si = cmul(sr, si, sr, si)
            qr, qi = cmul(qr, qi, qr, qi)
        t2r[0:8, cut], t2i[0:8, cut], t1r[0:8, cut], t1i[0:8, cut] = pr, pi, mr, mi
        done = 8
        while done < rows:
            more = min(done, rows - done)
            for off in range(0, more, 8):
                src, dst = slice(off, off + 8), slice(done + off, done + off + 8)
                t2r[dst, cut], t2i[dst, cut] = cmul(t2r[src, cut], t2i[src, cut], sr, si)
                t1r[dst, cut], t1i[dst, cut] = cmul(t1r[src, cut], t1i[src, cut], qr, qi)
            sr, si = cmul(sr, si, sr, si)
            qr, qi = cmul(qr, qi, qr, qi)
            done += more
        lastr, lasti = t2r[rows - 1 : rows, cut], t2i[rows - 1 : rows, cut]
        wr, wi = cmul(lastr, lasti, lr[0:1], li[0:1])
        l_ref[blk : blk + 1, :] = wr
        l_ref[n_blk + blk : n_blk + blk + 1, :] = wi
        l_ref[2 * n_blk + blk : 2 * n_blk + blk + 1, :] = lr[0:1]
        l_ref[3 * n_blk + blk : 3 * n_blk + blk + 1, :] = li[0:1]

    for copy in loads[:4]:
        copy.wait()
    keep_c = (
        lax.broadcasted_iota(jnp.int32, (LANES, lanes), 0) // group
        == lax.broadcasted_iota(jnp.int32, (LANES, lanes), 1) // state
    )
    for blk in range(n_blk):
        for part, in_ref, out_ref in ((0, bre, cre), (1, bim, cim)):
            at = slice(part * lanes, (part + 1) * lanes)
            ch = slice(blk * LANES, (blk + 1) * LANES)
            b, c = in_ref[ch, :], out_ref[ch, :]
            wide = jnp.where(keep_c, jnp.concatenate([b] * per, axis=1), 0.0)
            bs[blk, :, at] = wide.astype(BF16)
            wide = jnp.where(keep_c, jnp.concatenate([c if part == 0 else -c] * per, axis=1), 0.0)
            cs[blk, :, at] = wide.astype(BF16)
    lower = (
        lax.broadcasted_iota(jnp.int32, (rows, rows), 0)
        >= lax.broadcasted_iota(jnp.int32, (rows, rows), 1)
    ).astype(BF16)

    for k in range(1, n_tp):
        j = lax.rem(tp + k, n_tp)
        remote(nsend.at[j], urecv.at[j], a_send.at[k], a_recv.at[j], {"tp": j}).wait_recv()
    for j in range(n_tp):
        uf[j * mine : (j + 1) * mine, :] = urecv[j].astype(F32)
    ub[...] = uf[...].astype(BF16)

    for blk in range(n_blk):
        cut = slice(blk * lanes, (blk + 1) * lanes)
        u = ub[:, blk * LANES : (blk + 1) * LANES]
        d = jnp.dot(u, bs[blk], preferred_element_type=F32)
        wr, wi = cmul(d[:, :lanes], d[:, lanes:], t1r[:, cut], t1i[:, cut])
        wbuf[blk, :, :lanes] = wr.astype(BF16)
        wbuf[blk, :, lanes:] = wi.astype(BF16)
        er, ei = cmul(
            jnp.sum(wr, axis=0, keepdims=True), jnp.sum(wi, axis=0, keepdims=True),
            t2r[rows - 1 : rows, cut], t2i[rows - 1 : rows, cut],
        )
        e_f[blk : blk + 1, :] = er
        e_f[n_blk + blk : n_blk + blk + 1, :] = ei
    e_send[...] = e_f[...].astype(BF16)

    def end_copy(j):
        return remote(e_send, e_all.at[sp], e_ssem.at[j], e_rsem.at[sp], {"sp": j})

    def send_end(k, c):
        end_copy(n_sp - 1 - k).start()
        return c

    lax.fori_loop(0, n_sp - 1 - sp, send_end, 0)

    for blk in range(n_blk):
        cut = slice(blk * lanes, (blk + 1) * lanes)
        s = jnp.dot(lower, wbuf[blk], preferred_element_type=F32)
        xr, xi = cmul(s[:, :lanes], s[:, lanes:], t2r[:, cut], t2i[:, cut])
        wbuf[blk, :, :lanes] = xr.astype(BF16)
        wbuf[blk, :, lanes:] = xi.astype(BF16)
        y = lax.dot_general(wbuf[blk], cs[blk], NT, preferred_element_type=F32)
        ch = slice(blk * LANES, (blk + 1) * LANES)
        ylocal[:, ch] = y + skip[:, ch] * uf[:, ch]

    def join(j, held):
        hr, hi = held
        remote(e_send, e_all.at[j], e_ssem.at[j], e_rsem.at[j], {"sp": j}).wait_recv()
        e = e_all[j].astype(F32)
        hr, hi = cmul(hr, hi, l_ref[:n_blk], l_ref[n_blk : 2 * n_blk])
        return hr + e[:n_blk], hi + e[n_blk:]

    nil = jnp.zeros((n_blk, lanes), F32)
    hr, hi = lax.fori_loop(0, sp, join, (nil, nil))
    hr, hi = cmul(hr, hi, l_ref[2 * n_blk : 3 * n_blk], l_ref[3 * n_blk :])

    for blk in range(n_blk):
        cut = slice(blk * lanes, (blk + 1) * lanes)
        ch = slice(blk * LANES, (blk + 1) * LANES)
        xr, xi = cmul(hr[blk : blk + 1], hi[blk : blk + 1], t2r[:, cut], t2i[:, cut])
        wbuf[blk, :, :lanes] = xr.astype(BF16)
        wbuf[blk, :, lanes:] = xi.astype(BF16)
        y = lax.dot_general(wbuf[blk], cs[blk], NT, preferred_element_type=F32)
        zbuf[tp, blk] = jax.nn.gelu(y + ylocal[:, ch]).astype(BF16)
        for k in range(1, n_chip):
            j = lax.rem(tp + 2 * k, n_tp)
            copy = remote(
                zbuf.at[tp, blk], zbuf.at[tp, blk], z_send.at[k, blk], z_recv.at[tp, blk], {"tp": j}
            )
            copy.start()
            sends.append(copy)
        copy = remote(
            zbuf.at[tp, blk], zbuf.at[tp, blk], z_send.at[0, blk], z_recv.at[tp, blk], {"tp": partner}
        )
        copy.start()
        sends.append(copy)

    for copy in loads[4:]:
        copy.wait()

    def arrived(j, blk):
        remote(
            zbuf.at[j, blk], zbuf.at[j, blk], z_send.at[0, blk], z_recv.at[j, blk], {"tp": partner}
        ).wait_recv()

    def project(j, blk, first=False):
        at = pl.ds(pl.multiple_of(j * width + blk * LANES, LANES), LANES)
        z = zbuf[j, blk]
        v = jnp.dot(z, wv[at, :], preferred_element_type=F32)
        g = jnp.dot(z, wg[at, :], preferred_element_type=F32)
        if first:
            acc_v[...], acc_g[...] = v, g
        else:
            acc_v[...] += v
            acc_g[...] += g

    for blk in range(n_blk):
        project(tp, blk, blk == 0)
    for blk in range(n_blk):
        arrived(partner, blk)
        project(partner, blk)
    late = []
    for blk in range(n_blk):
        for k in range(1, n_chip):
            j = lax.rem(tp + n_tp - 2 * k, n_tp)
            arrived(j, blk)
            copy = remote(
                zbuf.at[j, blk], zbuf.at[j, blk], f_send.at[k, blk], z_recv.at[j, blk], {"tp": partner}
            )
            copy.start()
            sends.append(copy)
            project(j, blk)
            late.append((lax.rem(partner + n_tp - 2 * k, n_tp), blk))
            if len(late) > 1:
                item = late.pop(0)
                arrived(*item)
                project(*item)
    for item in late:
        arrived(*item)
        project(*item)

    gated = acc_v[...] * jax.nn.sigmoid(acc_g[...])
    acc_v[...] = gated
    square = gated * gated
    part = square[:, :LANES]
    for blk in range(1, n_blk):
        part = part + square[:, blk * LANES : (blk + 1) * LANES]
    total = lax.dot_general(jnp.ones((8, LANES), F32), part, NT, precision=HIGHEST, preferred_element_type=F32)
    sq_all[tp] = total[0:1]
    for k in range(1, n_tp):
        j = lax.rem(tp + n_tp - k, n_tp)
        copy = remote(sq_all.at[tp], sq_all.at[tp], q_send.at[k], q_recv.at[tp], {"tp": j})
        copy.start()
        sends.append(copy)
    total = total[0:1]
    for k in range(1, n_tp):
        j = lax.rem(tp + k, n_tp)
        remote(sq_all.at[j], sq_all.at[j], q_send.at[k], q_recv.at[j], {"tp": j}).wait_recv()
        total = total + sq_all[j]
    scale = lax.rsqrt(total / d_model + NORM_EPS)
    eye = (
        lax.broadcasted_iota(jnp.int32, (rows, rows), 0)
        == lax.broadcasted_iota(jnp.int32, (rows, rows), 1)
    ).astype(F32)
    column = lax.dot_general(
        eye, jnp.broadcast_to(scale, (LANES, rows)), NT, precision=HIGHEST, preferred_element_type=F32
    )
    for blk in range(n_blk):
        ch = slice(blk * LANES, (blk + 1) * LANES)
        out[:, ch] = (acc_v[:, ch] * column * nout[:, ch]).astype(BF16)

    for copy in sends:
        copy.wait_send()

    def sent(j, c):
        end_copy(j).wait_send()
        return c

    lax.fori_loop(sp + 1, n_sp, sent, 0)


def solution(mesh):
    n_sp, n_tp = mesh.shape["sp"], mesh.shape["tp"]

    def on_device(
        tokens, norm_in, decay_log, phase, b_real, b_imag, c_real, c_imag, skip_gain, w_value, w_gate, norm_out
    ):
        mine, d_model = tokens.shape
        rows = mine * n_tp
        groups, state, group = b_real.shape
        width = groups * group
        n_blk = width // LANES
        lanes = LANES // group * state
        entries = groups * state
        vmem = pl.BlockSpec(memory_space=pltpu.VMEM)
        hbm = pl.BlockSpec(memory_space=pl.ANY)
        dma = pltpu.SemaphoreType.DMA
        return pl.pallas_call(
            functools.partial(layer, n_sp, n_tp, state, group),
            out_shape=jax.ShapeDtypeStruct((rows, width), BF16),
            in_specs=[vmem] * 4 + [hbm] * 4 + [vmem] + [hbm] * 2 + [vmem],
            out_specs=vmem,
            scratch_shapes=[
                pltpu.VMEM((n_tp, mine, width), BF16),
                pltpu.VMEM((n_tp, mine, width), BF16),
                pltpu.VMEM((rows, width), F32),
                pltpu.VMEM((rows, width), BF16),
                pltpu.VMEM((8, entries), F32),
                pltpu.VMEM((8, entries), F32),
                pltpu.VMEM((rows, entries), F32),
                pltpu.VMEM((rows, entries), F32),
                pltpu.VMEM((rows, entries), F32),
                pltpu.VMEM((rows, entries), F32),
                pltpu.VMEM((n_blk, LANES, 2 * lanes), BF16),
                pltpu.VMEM((n_blk, LANES, 2 * lanes), BF16),
                pltpu.VMEM((n_blk, rows, 2 * lanes), BF16),
                pltpu.VMEM((rows, width), F32),
                pltpu.VMEM((2 * n_blk, lanes), F32),
                pltpu.VMEM((2 * n_blk, lanes), BF16),
                pltpu.VMEM((n_sp, 2 * n_blk, lanes), BF16),
                pltpu.VMEM((4 * n_blk, lanes), F32),
                pltpu.VMEM((n_tp, n_blk, rows, LANES), BF16),
                pltpu.VMEM(w_value.shape, BF16),
                pltpu.VMEM(w_gate.shape, BF16),
                pltpu.VMEM((rows, width), F32),
                pltpu.VMEM((rows, width), F32),
                pltpu.VMEM((n_tp, 1, rows), F32),
                pltpu.VMEM((width, state), F32),
                pltpu.VMEM((width, state), F32),
                pltpu.VMEM((width, state), F32),
                pltpu.VMEM((width, state), F32),
                dma((6,)),
                dma((n_tp,)),
                dma((n_tp,)),
                dma((n_sp,)),
                dma((n_sp,)),
                dma((n_tp // 2, n_blk)),
                dma((n_tp, n_blk)),
                dma((n_tp // 2, n_blk)),
                dma((n_tp,)),
                dma((n_tp,)),
            ],
            compiler_params=pltpu.CompilerParams(collective_id=0, has_side_effects=True),
        )(
            tokens,
            norm_in.reshape(1, -1),
            decay_log,
            phase,
            b_real.transpose(0, 2, 1).reshape(width, state),
            b_imag.transpose(0, 2, 1).reshape(width, state),
            c_real.reshape(width, state),
            c_imag.reshape(width, state),
            skip_gain.reshape(1, -1),
            w_value,
            w_gate,
            norm_out.reshape(1, -1),
        )

    placed = (
        P(("sp", "tp"), None),
        P(),
        P("tp", None),
        P("tp", None),
        P("tp", None, None),
        P("tp", None, None),
        P("tp", None, None),
        P("tp", None, None),
        P("tp"),
        P(None, "tp"),
        P(None, "tp"),
        P("tp"),
    )
    return jax.shard_map(
        on_device, mesh=mesh, in_specs=placed, out_specs=P("sp", "tp"), check_vma=False
    )
```

```python
import functools

import jax
import jax.numpy as jnp
from jax import lax
from jax.experimental import pallas as pl
from jax.experimental.pallas import tpu as pltpu
from jax.sharding import PartitionSpec as P

NORM_EPS = 1e-06
LANES = 128
F32 = jnp.float32
BF16 = jnp.bfloat16
HIGHEST = lax.Precision.HIGHEST
NT = (((1,), (1,)), ((), ()))


def cmul(ar, ai, br, bi):
    return ar * br - ai * bi, ar * bi + ai * br


def remote(src, dst, send, recv, target):
    return pltpu.make_async_remote_copy(
        src_ref=src,
        dst_ref=dst,
        send_sem=send,
        recv_sem=recv,
        device_id=target,
        device_id_type=pl.DeviceIdType.MESH,
    )


def layer(
    n_sp, n_tp, state, group,
    tok_h, nin_h, dlog_h, phase_h, bre_h, bim_h, cre_h, cim_h, skip_h, wv_h, wg_h, nout_h,
    out,
    nsend, urecv, uf, rows_a, rows_p, t1r, t1i, t2r, t2i, bs, cs, wbuf, ylocal,
    e_send, e_all, l_ref, zbuf, wv, wg, acc_v, acc_g, sq_all,
    bre, bim, cre, cim, tok, nin, dlog, phase, skip, nout,
    load_sem, a_send, a_recv, e_ssem, e_rsem, z_send, z_recv, f_send, q_send, q_recv,
):
    sp, tp = lax.axis_index("sp"), lax.axis_index("tp")
    mine, d_model = tok.shape
    rows, width = uf.shape
    n_blk = width // LANES
    per = LANES // group
    lanes = per * state
    core = lax.rem(tp, 2)
    partner = tp + 1 - 2 * core
    n_chip = n_tp // 2

    loads = [
        pltpu.make_async_copy(src, dst, load_sem.at[i])
        for i, (src, dst) in enumerate(
            (
                (tok_h, tok), (nin_h, nin), (dlog_h, dlog), (phase_h, phase),
                (bre_h, bre), (bim_h, bim), (cre_h, cre), (cim_h, cim),
                (skip_h, skip), (nout_h, nout), (wv_h, wv), (wg_h, wg),
            )
        )
    ]
    for copy in loads[:4]:
        copy.start()

    barrier = pltpu.get_barrier_semaphore()

    def greet(k, c):
        pl.semaphore_signal(
            barrier, inc=1, device_id={"sp": k}, device_id_type=pl.DeviceIdType.MESH
        )
        return c

    lax.fori_loop(0, sp, greet, 0)
    for k in range(1, n_tp):
        pl.semaphore_signal(
            barrier, inc=1, device_id={"tp": lax.rem(tp + k, n_tp)},
            device_id_type=pl.DeviceIdType.MESH,
        )
    for copy in loads[4:10]:
        copy.start()
    for copy in loads[:4]:
        copy.wait()

    xf = tok[...].astype(F32)
    scale = lax.rsqrt(jnp.sum(xf * xf, axis=1, keepdims=True) / d_model + NORM_EPS)
    normed = (xf * scale * nin[...]).astype(BF16)
    for j in range(n_tp):
        for blk in range(n_blk):
            at = j * width + blk * LANES
            nsend[j, blk] = normed[:, at : at + LANES]

    side = LANES // state
    for i in range(width // group // side):
        cut = slice(i * LANES, (i + 1) * LANES)
        for src, dst in ((dlog, rows_a), (phase, rows_p)):
            row = jnp.concatenate([src[i * side + k : i * side + k + 1, :] for k in range(side)], axis=1)
            dst[:, cut] = jnp.broadcast_to(row, (8, LANES))

    for blk in range(n_blk):
        cut = slice(blk * lanes, (blk + 1) * lanes)
        a, p = rows_a[:, cut], rows_p[:, cut]
        k = lax.broadcasted_iota(jnp.int32, a.shape, 0).astype(F32)
        mag, cos, sin = jnp.exp(a), jnp.cos(p), jnp.sin(p)
        lr, li = mag * cos, mag * sin
        inv = jnp.exp(-a)
        nr, ni = inv * cos, -inv * sin
        mod = a * a + p * p
        cr = ((lr - 1.0) * a + li * p) / mod
        ci = (li * a - (lr - 1.0) * p) / mod
        one, zero = jnp.ones_like(a), jnp.zeros_like(a)
        pr, pi, mr, mi = one, zero, cr, ci
        sr, si, qr, qi = lr, li, nr, ni
        row = lax.broadcasted_iota(jnp.int32, a.shape, 0)
        for bit in range(3):
            on = lax.rem(row // (1 << bit), 2) == 1
            ar, ai = cmul(pr, pi, sr, si)
            pr, pi = jnp.where(on, ar, pr), jnp.where(on, ai, pi)
            ar, ai = cmul(mr, mi, qr, qi)
            mr, mi = jnp.where(on, ar, mr), jnp.where(on, ai, mi)
            sr, si = cmul(sr, si, sr, si)
            qr, qi = cmul(qr, qi, qr, qi)
        t2r[0:8, cut], t2i[0:8, cut], t1r[0:8, cut], t1i[0:8, cut] = pr, pi, mr, mi
        done = 8
        while done < rows:
            more = min(done, rows - done)
            for off in range(0, more, 8):
                src, dst = slice(off, off + 8), slice(done + off, done + off + 8)
                t2r[dst, cut], t2i[dst, cut] = cmul(t2r[src, cut], t2i[src, cut], sr, si)
                t1r[dst, cut], t1i[dst, cut] = cmul(t1r[src, cut], t1i[src, cut], qr, qi)
            sr, si = cmul(sr, si, sr, si)
            qr, qi = cmul(qr, qi, qr, qi)
            done += more
        lastr, lasti = t2r[rows - 1 : rows, cut], t2i[rows - 1 : rows, cut]
        wr, wi = cmul(lastr, lasti, lr[0:1], li[0:1])
        l_ref[blk : blk + 1, :] = wr
        l_ref[n_blk + blk : n_blk + blk + 1, :] = wi
        l_ref[2 * n_blk + blk : 2 * n_blk + blk + 1, :] = lr[0:1]
        l_ref[3 * n_blk + blk : 3 * n_blk + blk + 1, :] = li[0:1]

    pl.semaphore_wait(barrier, n_tp - 1 + n_sp - 1 - sp)

    sends = []
    for blk in range(n_blk):
        for k in range(1, n_tp):
            j = lax.rem(tp + n_tp - k, n_tp)
            copy = remote(
                nsend.at[j, blk], urecv.at[tp, blk], a_send.at[k, blk], a_recv.at[tp, blk], {"tp": j}
            )
            copy.start()
            sends.append(copy)
    for copy in loads[10:]:
        copy.start()
    urecv[tp] = nsend[tp]

    for copy in loads[4:10]:
        copy.wait()
    keep_c = (
        lax.broadcasted_iota(jnp.int32, (LANES, lanes), 0) // group
        == lax.broadcasted_iota(jnp.int32, (LANES, lanes), 1) // state
    )
    for blk in range(n_blk):
        for part, in_ref, out_ref in ((0, bre, cre), (1, bim, cim)):
            at = slice(part * lanes, (part + 1) * lanes)
            ch = slice(blk * LANES, (blk + 1) * LANES)
            b, c = in_ref[ch, :], out_ref[ch, :]
            wide = jnp.where(keep_c, jnp.concatenate([b] * per, axis=1), 0.0)
            bs[blk, :, at] = wide.astype(BF16)
            wide = jnp.where(keep_c, jnp.concatenate([c if part == 0 else -c] * per, axis=1), 0.0)
            cs[blk, :, at] = wide.astype(BF16)
    lower = (
        lax.broadcasted_iota(jnp.int32, (rows, rows), 0)
        >= lax.broadcasted_iota(jnp.int32, (rows, rows), 1)
    ).astype(BF16)

    def end_copy(j, blk):
        return remote(
            e_send.at[blk], e_all.at[sp, blk], e_ssem.at[j, blk], e_rsem.at[sp, blk], {"sp": j}
        )

    for blk in range(n_blk):
        cut = slice(blk * lanes, (blk + 1) * lanes)
        ch = slice(blk * LANES, (blk + 1) * LANES)
        for k in range(1, n_tp):
            j = lax.rem(tp + k, n_tp)
            remote(
                nsend.at[j, blk], urecv.at[j, blk], a_send.at[k, blk], a_recv.at[j, blk], {"tp": j}
            ).wait_recv()
        for j in range(n_tp):
            uf[j * mine : (j + 1) * mine, ch] = urecv[j, blk].astype(F32)
        u = uf[:, ch].astype(BF16)
        d = jnp.dot(u, bs[blk], preferred_element_type=F32)
        wr, wi = cmul(d[:, :lanes], d[:, lanes:], t1r[:, cut], t1i[:, cut])
        wbuf[blk, :, :lanes] = wr.astype(BF16)
        wbuf[blk, :, lanes:] = wi.astype(BF16)
        er, ei = cmul(
            jnp.sum(wr, axis=0, keepdims=True), jnp.sum(wi, axis=0, keepdims=True),
            t2r[rows - 1 : rows, cut], t2i[rows - 1 : rows, cut],
        )
        e_send[blk] = jnp.concatenate([er, ei], axis=0).astype(BF16)

        def send_end(k, c, blk=blk):
            end_copy(n_sp - 1 - k, blk).start()
            return c

        lax.fori_loop(0, n_sp - 1 - sp, send_end, 0)

    for blk in range(n_blk):
        cut = slice(blk * lanes, (blk + 1) * lanes)
        s = jnp.dot(lower, wbuf[blk], preferred_element_type=F32)
        xr, xi = cmul(s[:, :lanes], s[:, lanes:], t2r[:, cut], t2i[:, cut])
        wbuf[blk, :, :lanes] = xr.astype(BF16)
        wbuf[blk, :, lanes:] = xi.astype(BF16)
        y = lax.dot_general(wbuf[blk], cs[blk], NT, preferred_element_type=F32)
        ch = slice(blk * LANES, (blk + 1) * LANES)
        ylocal[:, ch] = y + skip[:, ch] * uf[:, ch]

    for blk in range(n_blk):
        cut = slice(blk * lanes, (blk + 1) * lanes)
        ch = slice(blk * LANES, (blk + 1) * LANES)
        lr, li = l_ref[blk : blk + 1, :], l_ref[n_blk + blk : n_blk + blk + 1, :]

        def join(j, held, blk=blk, lr=lr, li=li):
            remote(
                e_send.at[blk], e_all.at[j, blk], e_ssem.at[j, blk], e_rsem.at[j, blk], {"sp": j}
            ).wait_recv()
            e = e_all[j, blk].astype(F32)
            hr, hi = cmul(*held, lr, li)
            return hr + e[0:1], hi + e[1:2]

        nil = jnp.zeros((1, lanes), F32)
        hr, hi = lax.fori_loop(0, sp, join, (nil, nil))
        hr, hi = cmul(
            hr, hi, l_ref[2 * n_blk + blk : 2 * n_blk + blk + 1, :], l_ref[3 * n_blk + blk : 3 * n_blk + blk + 1, :]
        )
        xr, xi = cmul(hr, hi, t2r[:, cut], t2i[:, cut])
        wbuf[blk, :, :lanes] = xr.astype(BF16)
        wbuf[blk, :, lanes:] = xi.astype(BF16)
        y = lax.dot_general(wbuf[blk], cs[blk], NT, preferred_element_type=F32)
        zbuf[tp, blk] = jax.nn.gelu(y + ylocal[:, ch]).astype(BF16)
        for k in range(1, n_chip):
            j = lax.rem(tp + 2 * k, n_tp)
            copy = remote(
                zbuf.at[tp, blk], zbuf.at[tp, blk], z_send.at[k, blk], z_recv.at[tp, blk], {"tp": j}
            )
            copy.start()
            sends.append(copy)
        copy = remote(
            zbuf.at[tp, blk], zbuf.at[tp, blk], z_send.at[0, blk], z_recv.at[tp, blk], {"tp": partner}
        )
        copy.start()
        sends.append(copy)

    for copy in loads[10:]:
        copy.wait()

    def arrived(j, blk):
        remote(
            zbuf.at[j, blk], zbuf.at[j, blk], z_send.at[0, blk], z_recv.at[j, blk], {"tp": partner}
        ).wait_recv()

    def project(j, blk, first=False):
        at = pl.ds(pl.multiple_of(j * width + blk * LANES, LANES), LANES)
        z = zbuf[j, blk]
        v = jnp.dot(z, wv[at, :], preferred_element_type=F32)
        g = jnp.dot(z, wg[at, :], preferred_element_type=F32)
        if first:
            acc_v[...], acc_g[...] = v, g
        else:
            acc_v[...] += v
            acc_g[...] += g

    for blk in range(n_blk):
        project(tp, blk, blk == 0)
    for blk in range(n_blk):
        arrived(partner, blk)
        project(partner, blk)
    late = []
    for blk in range(n_blk):
        for k in range(1, n_chip):
            j = lax.rem(tp + n_tp - 2 * k, n_tp)
            arrived(j, blk)
            copy = remote(
                zbuf.at[j, blk], zbuf.at[j, blk], f_send.at[k, blk], z_recv.at[j, blk], {"tp": partner}
            )
            copy.start()
            sends.append(copy)
            project(j, blk)
            late.append((lax.rem(partner + n_tp - 2 * k, n_tp), blk))
            if len(late) > 1:
                item = late.pop(0)
                arrived(*item)
                project(*item)
    for item in late:
        arrived(*item)
        project(*item)

    gated = acc_v[...] * jax.nn.sigmoid(acc_g[...])
    acc_v[...] = gated
    square = gated * gated
    part = square[:, :LANES]
    for blk in range(1, n_blk):
        part = part + square[:, blk * LANES : (blk + 1) * LANES]
    total = lax.dot_general(jnp.ones((8, LANES), F32), part, NT, precision=HIGHEST, preferred_element_type=F32)
    sq_all[tp] = total[0:1]
    for k in range(1, n_tp):
        j = lax.rem(tp + n_tp - k, n_tp)
        copy = remote(sq_all.at[tp], sq_all.at[tp], q_send.at[k], q_recv.at[tp], {"tp": j})
        copy.start()
        sends.append(copy)
    total = total[0:1]
    for k in range(1, n_tp):
        j = lax.rem(tp + k, n_tp)
        remote(sq_all.at[j], sq_all.at[j], q_send.at[k], q_recv.at[j], {"tp": j}).wait_recv()
        total = total + sq_all[j]
    scale = lax.rsqrt(total / d_model + NORM_EPS)
    eye = (
        lax.broadcasted_iota(jnp.int32, (rows, rows), 0)
        == lax.broadcasted_iota(jnp.int32, (rows, rows), 1)
    ).astype(F32)
    column = lax.dot_general(
        eye, jnp.broadcast_to(scale, (LANES, rows)), NT, precision=HIGHEST, preferred_element_type=F32
    )
    for blk in range(n_blk):
        ch = slice(blk * LANES, (blk + 1) * LANES)
        out[:, ch] = (acc_v[:, ch] * column * nout[:, ch]).astype(BF16)

    for copy in sends:
        copy.wait_send()

    def sent(j, c):
        for blk in range(n_blk):
            end_copy(j, blk).wait_send()
        return c

    lax.fori_loop(sp + 1, n_sp, sent, 0)


def solution(mesh):
    n_sp, n_tp = mesh.shape["sp"], mesh.shape["tp"]

    def on_device(
        tokens, norm_in, decay_log, phase, b_real, b_imag, c_real, c_imag, skip_gain, w_value, w_gate, norm_out
    ):
        mine, d_model = tokens.shape
        rows = mine * n_tp
        groups, state, group = b_real.shape
        width = groups * group
        n_blk = width // LANES
        lanes = LANES // group * state
        entries = groups * state
        vmem = pl.BlockSpec(memory_space=pltpu.VMEM)
        hbm = pl.BlockSpec(memory_space=pl.ANY)
        dma = pltpu.SemaphoreType.DMA
        return pl.pallas_call(
            functools.partial(layer, n_sp, n_tp, state, group),
            out_shape=jax.ShapeDtypeStruct((rows, width), BF16),
            in_specs=[hbm] * 12,
            out_specs=vmem,
            scratch_shapes=[
                pltpu.VMEM((n_tp, n_blk, mine, LANES), BF16),
                pltpu.VMEM((n_tp, n_blk, mine, LANES), BF16),
                pltpu.VMEM((rows, width), F32),
                pltpu.VMEM((8, entries), F32),
                pltpu.VMEM((8, entries), F32),
                pltpu.VMEM((rows, entries), F32),
                pltpu.VMEM((rows, entries), F32),
                pltpu.VMEM((rows, entries), F32),
                pltpu.VMEM((rows, entries), F32),
                pltpu.VMEM((n_blk, LANES, 2 * lanes), BF16),
                pltpu.VMEM((n_blk, LANES, 2 * lanes), BF16),
                pltpu.VMEM((n_blk, rows, 2 * lanes), BF16),
                pltpu.VMEM((rows, width), F32),
                pltpu.VMEM((n_blk, 2, lanes), BF16),
                pltpu.VMEM((n_sp, n_blk, 2, lanes), BF16),
                pltpu.VMEM((4 * n_blk, lanes), F32),
                pltpu.VMEM((n_tp, n_blk, rows, LANES), BF16),
                pltpu.VMEM(w_value.shape, BF16),
                pltpu.VMEM(w_gate.shape, BF16),
                pltpu.VMEM((rows, width), F32),
                pltpu.VMEM((rows, width), F32),
                pltpu.VMEM((n_tp, 1, rows), F32),
                pltpu.VMEM((width, state), F32),
                pltpu.VMEM((width, state), F32),
                pltpu.VMEM((width, state), F32),
                pltpu.VMEM((width, state), F32),
                pltpu.VMEM((mine, d_model), BF16),
                pltpu.VMEM((1, d_model), F32),
                pltpu.VMEM((groups, state), F32),
                pltpu.VMEM((groups, state), F32),
                pltpu.VMEM((1, width), F32),
                pltpu.VMEM((1, width), F32),
                dma((12,)),
                dma((n_tp, n_blk)),
                dma((n_tp, n_blk)),
                dma((n_sp, n_blk)),
                dma((n_sp, n_blk)),
                dma((n_tp // 2, n_blk)),
                dma((n_tp, n_blk)),
                dma((n_tp // 2, n_blk)),
                dma((n_tp,)),
                dma((n_tp,)),
            ],
            compiler_params=pltpu.CompilerParams(collective_id=0, has_side_effects=True),
        )(
            tokens,
            norm_in.reshape(1, -1),
            decay_log,
            phase,
            b_real.transpose(0, 2, 1).reshape(width, state),
            b_imag.transpose(0, 2, 1).reshape(width, state),
            c_real.reshape(width, state),
            c_imag.reshape(width, state),
            skip_gain.reshape(1, -1),
            w_value,
            w_gate,
            norm_out.reshape(1, -1),
        )

    placed = (
        P(("sp", "tp"), None),
        P(),
        P("tp", None),
        P("tp", None),
        P("tp", None, None),
        P("tp", None, None),
        P("tp", None, None),
        P("tp", None, None),
        P("tp"),
        P(None, "tp"),
        P(None, "tp"),
        P("tp"),
    )
    return jax.shard_map(
        on_device, mesh=mesh, in_specs=placed, out_specs=P("sp", "tp"), check_vma=False
    )
```

```python
import functools

import jax
import jax.numpy as jnp
from jax import lax
from jax.experimental import pallas as pl
from jax.experimental.pallas import tpu as pltpu
from jax.sharding import PartitionSpec as P

NORM_EPS = 1e-06
LANES = 128
F32 = jnp.float32
BF16 = jnp.bfloat16
HIGHEST = lax.Precision.HIGHEST
NT = (((1,), (1,)), ((), ()))


def cmul(ar, ai, br, bi):
    return ar * br - ai * bi, ar * bi + ai * br


def remote(src, dst, send, recv, target):
    return pltpu.make_async_remote_copy(
        src_ref=src,
        dst_ref=dst,
        send_sem=send,
        recv_sem=recv,
        device_id=target,
        device_id_type=pl.DeviceIdType.MESH,
    )


def layer(
    n_sp, n_tp, state, group,
    tok_h, nin_h, dlog_h, phase_h, bre_h, bim_h, cre_h, cim_h, skip_h, wv_h, wg_h, nout_h,
    out,
    nsend, urecv, uf, rows_a, rows_p, t1r, t1i, t2r, t2i, bs, cs, wbuf, ylocal,
    e_send, e_all, l_ref, zbuf, wv, wg, acc_v, acc_g, sq_all,
    bre, bim, cre, cim, tok, nin, dlog, phase, skip, nout,
    load_sem, a_send, a_recv, e_ssem, e_rsem, z_send, z_recv, f_send, q_send, q_recv, met,
):
    sp, tp = lax.axis_index("sp"), lax.axis_index("tp")
    mine, d_model = tok.shape
    rows, width = uf.shape
    n_blk = width // LANES
    per = LANES // group
    lanes = per * state
    core = lax.rem(tp, 2)
    partner = tp + 1 - 2 * core
    n_chip = n_tp // 2

    loads = [
        pltpu.make_async_copy(src, dst, load_sem.at[i])
        for i, (src, dst) in enumerate(
            (
                (tok_h, tok), (nin_h, nin), (dlog_h, dlog), (phase_h, phase),
                (bre_h, bre), (bim_h, bim), (cre_h, cre), (cim_h, cim),
                (skip_h, skip), (nout_h, nout), (wv_h, wv), (wg_h, wg),
            )
        )
    ]
    for copy in loads[:4]:
        copy.start()

    barrier = pltpu.get_barrier_semaphore()

    def signal_sp(sem, d):
        for ok, to in ((sp >= d, sp - d), (sp + d < n_sp, sp + d)):

            @pl.when(ok)
            def _(to=to):
                pl.semaphore_signal(
                    sem, inc=1, device_id={"sp": to}, device_id_type=pl.DeviceIdType.MESH
                )

    def around(d):
        return jnp.where(sp >= d, 1, 0) + jnp.where(sp + d < n_sp, 1, 0)

    signal_sp(barrier, 1)
    for k in range(1, n_tp):
        pl.semaphore_signal(
            barrier, inc=1, device_id={"tp": lax.rem(tp + k, n_tp)},
            device_id_type=pl.DeviceIdType.MESH,
        )
    for copy in loads[4:10]:
        copy.start()
    for copy in loads[:4]:
        copy.wait()

    xf = tok[...].astype(F32)
    scale = lax.rsqrt(jnp.sum(xf * xf, axis=1, keepdims=True) / d_model + NORM_EPS)
    normed = (xf * scale * nin[...]).astype(BF16)
    for j in range(n_tp):
        for blk in range(n_blk):
            at = j * width + blk * LANES
            nsend[j, blk] = normed[:, at : at + LANES]

    side = LANES // state
    for i in range(width // group // side):
        cut = slice(i * LANES, (i + 1) * LANES)
        for src, dst in ((dlog, rows_a), (phase, rows_p)):
            row = jnp.concatenate([src[i * side + k : i * side + k + 1, :] for k in range(side)], axis=1)
            dst[:, cut] = jnp.broadcast_to(row, (8, LANES))

    for blk in range(n_blk):
        cut = slice(blk * lanes, (blk + 1) * lanes)
        a, p = rows_a[:, cut], rows_p[:, cut]
        k = lax.broadcasted_iota(jnp.int32, a.shape, 0).astype(F32)
        mag, cos, sin = jnp.exp(a), jnp.cos(p), jnp.sin(p)
        lr, li = mag * cos, mag * sin
        inv = jnp.exp(-a)
        nr, ni = inv * cos, -inv * sin
        mod = a * a + p * p
        cr = ((lr - 1.0) * a + li * p) / mod
        ci = (li * a - (lr - 1.0) * p) / mod
        one, zero = jnp.ones_like(a), jnp.zeros_like(a)
        pr, pi, mr, mi = one, zero, cr, ci
        sr, si, qr, qi = lr, li, nr, ni
        row = lax.broadcasted_iota(jnp.int32, a.shape, 0)
        for bit in range(3):
            on = lax.rem(row // (1 << bit), 2) == 1
            ar, ai = cmul(pr, pi, sr, si)
            pr, pi = jnp.where(on, ar, pr), jnp.where(on, ai, pi)
            ar, ai = cmul(mr, mi, qr, qi)
            mr, mi = jnp.where(on, ar, mr), jnp.where(on, ai, mi)
            sr, si = cmul(sr, si, sr, si)
            qr, qi = cmul(qr, qi, qr, qi)
        t2r[0:8, cut], t2i[0:8, cut], t1r[0:8, cut], t1i[0:8, cut] = pr, pi, mr, mi
        done = 8
        while done < rows:
            more = min(done, rows - done)
            for off in range(0, more, 8):
                src, dst = slice(off, off + 8), slice(done + off, done + off + 8)
                t2r[dst, cut], t2i[dst, cut] = cmul(t2r[src, cut], t2i[src, cut], sr, si)
                t1r[dst, cut], t1i[dst, cut] = cmul(t1r[src, cut], t1i[src, cut], qr, qi)
            sr, si = cmul(sr, si, sr, si)
            qr, qi = cmul(qr, qi, qr, qi)
            done += more
        lastr, lasti = t2r[rows - 1 : rows, cut], t2i[rows - 1 : rows, cut]
        wr, wi = cmul(lastr, lasti, lr[0:1], li[0:1])
        l_ref[blk : blk + 1, :] = wr
        l_ref[n_blk + blk : n_blk + blk + 1, :] = wi
        l_ref[2 * n_blk + blk : 2 * n_blk + blk + 1, :] = lr[0:1]
        l_ref[3 * n_blk + blk : 3 * n_blk + blk + 1, :] = li[0:1]

    pl.semaphore_wait(barrier, n_tp - 1 + around(1))

    sends = []
    for blk in range(n_blk):
        for k in range(1, n_tp):
            j = lax.rem(tp + n_tp - k, n_tp)
            copy = remote(
                nsend.at[j, blk], urecv.at[tp, blk], a_send.at[k, blk], a_recv.at[tp, blk], {"tp": j}
            )
            copy.start()
            sends.append(copy)
    if n_sp > 2:
        signal_sp(met.at[0], 1)
    for copy in loads[10:]:
        copy.start()
    urecv[tp] = nsend[tp]

    for copy in loads[4:10]:
        copy.wait()
    keep_c = (
        lax.broadcasted_iota(jnp.int32, (LANES, lanes), 0) // group
        == lax.broadcasted_iota(jnp.int32, (LANES, lanes), 1) // state
    )
    for blk in range(n_blk):
        for part, in_ref, out_ref in ((0, bre, cre), (1, bim, cim)):
            at = slice(part * lanes, (part + 1) * lanes)
            ch = slice(blk * LANES, (blk + 1) * LANES)
            b, c = in_ref[ch, :], out_ref[ch, :]
            wide = jnp.where(keep_c, jnp.concatenate([b] * per, axis=1), 0.0)
            bs[blk, :, at] = wide.astype(BF16)
            wide = jnp.where(keep_c, jnp.concatenate([c if part == 0 else -c] * per, axis=1), 0.0)
            cs[blk, :, at] = wide.astype(BF16)
    lower = (
        lax.broadcasted_iota(jnp.int32, (rows, rows), 0)
        >= lax.broadcasted_iota(jnp.int32, (rows, rows), 1)
    ).astype(BF16)

    d = 1
    hops = []
    while d < n_sp - 1:
        hops.append(d)
        d *= 2
    for r, d in enumerate(hops):
        if r > 0:
            signal_sp(met.at[r], d)
        pl.semaphore_wait(met.at[r], around(d))

    def end_copy(j, blk):
        return remote(
            e_send.at[blk], e_all.at[sp, blk], e_ssem.at[j, blk], e_rsem.at[sp, blk], {"sp": j}
        )

    for blk in range(n_blk):
        cut = slice(blk * lanes, (blk + 1) * lanes)
        ch = slice(blk * LANES, (blk + 1) * LANES)
        for k in range(1, n_tp):
            j = lax.rem(tp + k, n_tp)
            remote(
                nsend.at[j, blk], urecv.at[j, blk], a_send.at[k, blk], a_recv.at[j, blk], {"tp": j}
            ).wait_recv()
        for j in range(n_tp):
            uf[j * mine : (j + 1) * mine, ch] = urecv[j, blk].astype(F32)
        u = uf[:, ch].astype(BF16)
        d = jnp.dot(u, bs[blk], preferred_element_type=F32)
        wr, wi = cmul(d[:, :lanes], d[:, lanes:], t1r[:, cut], t1i[:, cut])
        wbuf[blk, :, :lanes] = wr.astype(BF16)
        wbuf[blk, :, lanes:] = wi.astype(BF16)
        er, ei = cmul(
            jnp.sum(wr, axis=0, keepdims=True), jnp.sum(wi, axis=0, keepdims=True),
            t2r[rows - 1 : rows, cut], t2i[rows - 1 : rows, cut],
        )
        e_send[blk] = jnp.concatenate([er, ei], axis=0).astype(BF16)

        def send_end(k, c, blk=blk):
            end_copy(n_sp - 1 - k, blk).start()
            return c

        lax.fori_loop(0, n_sp - 1 - sp, send_end, 0)

    for blk in range(n_blk):
        cut = slice(blk * lanes, (blk + 1) * lanes)
        s = jnp.dot(lower, wbuf[blk], preferred_element_type=F32)
        xr, xi = cmul(s[:, :lanes], s[:, lanes:], t2r[:, cut], t2i[:, cut])
        wbuf[blk, :, :lanes] = xr.astype(BF16)
        wbuf[blk, :, lanes:] = xi.astype(BF16)
        y = lax.dot_general(wbuf[blk], cs[blk], NT, preferred_element_type=F32)
        ch = slice(blk * LANES, (blk + 1) * LANES)
        ylocal[:, ch] = y + skip[:, ch] * uf[:, ch]

    for blk in range(n_blk):
        cut = slice(blk * lanes, (blk + 1) * lanes)
        ch = slice(blk * LANES, (blk + 1) * LANES)
        lr, li = l_ref[blk : blk + 1, :], l_ref[n_blk + blk : n_blk + blk + 1, :]

        def join(j, held, blk=blk, lr=lr, li=li):
            remote(
                e_send.at[blk], e_all.at[j, blk], e_ssem.at[j, blk], e_rsem.at[j, blk], {"sp": j}
            ).wait_recv()
            e = e_all[j, blk].astype(F32)
            hr, hi = cmul(*held, lr, li)
            return hr + e[0:1], hi + e[1:2]

        nil = jnp.zeros((1, lanes), F32)
        hr, hi = lax.fori_loop(0, sp, join, (nil, nil))
        hr, hi = cmul(
            hr, hi, l_ref[2 * n_blk + blk : 2 * n_blk + blk + 1, :], l_ref[3 * n_blk + blk : 3 * n_blk + blk + 1, :]
        )
        xr, xi = cmul(hr, hi, t2r[:, cut], t2i[:, cut])
        wbuf[blk, :, :lanes] = xr.astype(BF16)
        wbuf[blk, :, lanes:] = xi.astype(BF16)
        y = lax.dot_general(wbuf[blk], cs[blk], NT, preferred_element_type=F32)
        zbuf[tp, blk] = jax.nn.gelu(y + ylocal[:, ch]).astype(BF16)
        for k in range(1, n_chip):
            j = lax.rem(tp + 2 * k, n_tp)
            copy = remote(
                zbuf.at[tp, blk], zbuf.at[tp, blk], z_send.at[k, blk], z_recv.at[tp, blk], {"tp": j}
            )
            copy.start()
            sends.append(copy)
        copy = remote(
            zbuf.at[tp, blk], zbuf.at[tp, blk], z_send.at[0, blk], z_recv.at[tp, blk], {"tp": partner}
        )
        copy.start()
        sends.append(copy)

    for copy in loads[10:]:
        copy.wait()

    def arrived(j, blk):
        remote(
            zbuf.at[j, blk], zbuf.at[j, blk], z_send.at[0, blk], z_recv.at[j, blk], {"tp": partner}
        ).wait_recv()

    def project(j, blk, first=False):
        at = pl.ds(pl.multiple_of(j * width + blk * LANES, LANES), LANES)
        z = zbuf[j, blk]
        v = jnp.dot(z, wv[at, :], preferred_element_type=F32)
        g = jnp.dot(z, wg[at, :], preferred_element_type=F32)
        if first:
            acc_v[...], acc_g[...] = v, g
        else:
            acc_v[...] += v
            acc_g[...] += g

    for blk in range(n_blk):
        project(tp, blk, blk == 0)
    for blk in range(n_blk):
        arrived(partner, blk)
        project(partner, blk)
    late = []
    for blk in range(n_blk):
        for k in range(1, n_chip):
            j = lax.rem(tp + n_tp - 2 * k, n_tp)
            arrived(j, blk)
            copy = remote(
                zbuf.at[j, blk], zbuf.at[j, blk], f_send.at[k, blk], z_recv.at[j, blk], {"tp": partner}
            )
            copy.start()
            sends.append(copy)
            project(j, blk)
            late.append((lax.rem(partner + n_tp - 2 * k, n_tp), blk))
            if len(late) > 1:
                item = late.pop(0)
                arrived(*item)
                project(*item)
    for item in late:
        arrived(*item)
        project(*item)

    gated = acc_v[...] * jax.nn.sigmoid(acc_g[...])
    acc_v[...] = gated
    square = gated * gated
    part = square[:, :LANES]
    for blk in range(1, n_blk):
        part = part + square[:, blk * LANES : (blk + 1) * LANES]
    total = lax.dot_general(jnp.ones((8, LANES), F32), part, NT, precision=HIGHEST, preferred_element_type=F32)
    sq_all[tp] = total[0:1]
    for k in range(1, n_tp):
        j = lax.rem(tp + n_tp - k, n_tp)
        copy = remote(sq_all.at[tp], sq_all.at[tp], q_send.at[k], q_recv.at[tp], {"tp": j})
        copy.start()
        sends.append(copy)
    total = total[0:1]
    for k in range(1, n_tp):
        j = lax.rem(tp + k, n_tp)
        remote(sq_all.at[j], sq_all.at[j], q_send.at[k], q_recv.at[j], {"tp": j}).wait_recv()
        total = total + sq_all[j]
    scale = lax.rsqrt(total / d_model + NORM_EPS)
    eye = (
        lax.broadcasted_iota(jnp.int32, (rows, rows), 0)
        == lax.broadcasted_iota(jnp.int32, (rows, rows), 1)
    ).astype(F32)
    column = lax.dot_general(
        eye, jnp.broadcast_to(scale, (LANES, rows)), NT, precision=HIGHEST, preferred_element_type=F32
    )
    for blk in range(n_blk):
        ch = slice(blk * LANES, (blk + 1) * LANES)
        out[:, ch] = (acc_v[:, ch] * column * nout[:, ch]).astype(BF16)

    for copy in sends:
        copy.wait_send()

    def sent(j, c):
        for blk in range(n_blk):
            end_copy(j, blk).wait_send()
        return c

    lax.fori_loop(sp + 1, n_sp, sent, 0)


def solution(mesh):
    n_sp, n_tp = mesh.shape["sp"], mesh.shape["tp"]

    def on_device(
        tokens, norm_in, decay_log, phase, b_real, b_imag, c_real, c_imag, skip_gain, w_value, w_gate, norm_out
    ):
        mine, d_model = tokens.shape
        rows = mine * n_tp
        groups, state, group = b_real.shape
        width = groups * group
        n_blk = width // LANES
        lanes = LANES // group * state
        entries = groups * state
        vmem = pl.BlockSpec(memory_space=pltpu.VMEM)
        hbm = pl.BlockSpec(memory_space=pl.ANY)
        dma = pltpu.SemaphoreType.DMA
        return pl.pallas_call(
            functools.partial(layer, n_sp, n_tp, state, group),
            out_shape=pltpu.VMEM((rows, width), BF16),
            in_specs=[hbm] * 12,
            out_specs=vmem,
            scratch_shapes=[
                pltpu.VMEM((n_tp, n_blk, mine, LANES), BF16),
                pltpu.VMEM((n_tp, n_blk, mine, LANES), BF16),
                pltpu.VMEM((rows, width), F32),
                pltpu.VMEM((8, entries), F32),
                pltpu.VMEM((8, entries), F32),
                pltpu.VMEM((rows, entries), F32),
                pltpu.VMEM((rows, entries), F32),
                pltpu.VMEM((rows, entries), F32),
                pltpu.VMEM((rows, entries), F32),
                pltpu.VMEM((n_blk, LANES, 2 * lanes), BF16),
                pltpu.VMEM((n_blk, LANES, 2 * lanes), BF16),
                pltpu.VMEM((n_blk, rows, 2 * lanes), BF16),
                pltpu.VMEM((rows, width), F32),
                pltpu.VMEM((n_blk, 2, lanes), BF16),
                pltpu.VMEM((n_sp, n_blk, 2, lanes), BF16),
                pltpu.VMEM((4 * n_blk, lanes), F32),
                pltpu.VMEM((n_tp, n_blk, rows, LANES), BF16),
                pltpu.VMEM(w_value.shape, BF16),
                pltpu.VMEM(w_gate.shape, BF16),
                pltpu.VMEM((rows, width), F32),
                pltpu.VMEM((rows, width), F32),
                pltpu.VMEM((n_tp, 1, rows), F32),
                pltpu.VMEM((width, state), F32),
                pltpu.VMEM((width, state), F32),
                pltpu.VMEM((width, state), F32),
                pltpu.VMEM((width, state), F32),
                pltpu.VMEM((mine, d_model), BF16),
                pltpu.VMEM((1, d_model), F32),
                pltpu.VMEM((groups, state), F32),
                pltpu.VMEM((groups, state), F32),
                pltpu.VMEM((1, width), F32),
                pltpu.VMEM((1, width), F32),
                dma((12,)),
                dma((n_tp, n_blk)),
                dma((n_tp, n_blk)),
                dma((n_sp, n_blk)),
                dma((n_sp, n_blk)),
                dma((n_tp // 2, n_blk)),
                dma((n_tp, n_blk)),
                dma((n_tp // 2, n_blk)),
                dma((n_tp,)),
                dma((n_tp,)),
                pltpu.SemaphoreType.REGULAR((max(n_sp.bit_length(), 1),)),
            ],
            compiler_params=pltpu.CompilerParams(collective_id=0, has_side_effects=True),
        )(
            tokens,
            norm_in.reshape(1, -1),
            decay_log,
            phase,
            b_real.transpose(0, 2, 1).reshape(width, state),
            b_imag.transpose(0, 2, 1).reshape(width, state),
            c_real.reshape(width, state),
            c_imag.reshape(width, state),
            skip_gain.reshape(1, -1),
            w_value,
            w_gate,
            norm_out.reshape(1, -1),
        )

    placed = (
        P(("sp", "tp"), None),
        P(),
        P("tp", None),
        P("tp", None),
        P("tp", None, None),
        P("tp", None, None),
        P("tp", None, None),
        P("tp", None, None),
        P("tp"),
        P(None, "tp"),
        P(None, "tp"),
        P("tp"),
    )
    return jax.shard_map(
        on_device, mesh=mesh, in_specs=placed, out_specs=P("sp", "tp"), check_vma=False
    )
```

```python
import functools

import jax
import jax.numpy as jnp
from jax import lax
from jax.experimental import pallas as pl
from jax.experimental.pallas import tpu as pltpu
from jax.sharding import PartitionSpec as P

NORM_EPS = 1e-06
LANES = 128
F32 = jnp.float32
BF16 = jnp.bfloat16
NT = (((1,), (1,)), ((), ()))


def cmul(ar, ai, br, bi):
    return ar * br - ai * bi, ar * bi + ai * br


def exact(ones, value):
    total = None
    for _ in range(3):
        term = value.astype(BF16)
        value = value - term.astype(F32)
        dot = lax.dot_general(ones, term, NT, preferred_element_type=F32)
        total = dot if total is None else total + dot
    return total


def remote(src, dst, send, recv, target):
    return pltpu.make_async_remote_copy(
        src_ref=src,
        dst_ref=dst,
        send_sem=send,
        recv_sem=recv,
        device_id=target,
        device_id_type=pl.DeviceIdType.MESH,
    )


def layer(
    n_sp, n_tp, state, group,
    tok_h, nin_h, dlog_h, phase_h, bre_h, bim_h, cre_h, cim_h, skip_h, wv_h, wg_h, nout_h,
    out,
    nsend, urecv, uf, rows_a, rows_p, t1r, t1i, t2r, t2i, bs, cs, wbuf, ylocal,
    e_send, e_all, l_ref, zbuf, wv, wg, acc_v, acc_g, sq_all,
    bre, bim, cre, cim, tok, nin, dlog, phase, skip, nout,
    load_sem, a_send, a_recv, e_ssem, e_rsem, z_send, z_recv, f_send, q_send, q_recv, met,
):
    sp, tp = lax.axis_index("sp"), lax.axis_index("tp")
    mine, d_model = tok.shape
    rows, width = uf.shape
    n_blk = width // LANES
    per = LANES // group
    lanes = per * state
    core = lax.rem(tp, 2)
    partner = tp + 1 - 2 * core
    n_chip = n_tp // 2

    loads = [
        pltpu.make_async_copy(src, dst, load_sem.at[i])
        for i, (src, dst) in enumerate(
            (
                (tok_h, tok), (nin_h, nin), (dlog_h, dlog), (phase_h, phase),
                (bre_h, bre), (bim_h, bim), (cre_h, cre), (cim_h, cim),
                (skip_h, skip), (nout_h, nout), (wv_h, wv), (wg_h, wg),
            )
        )
    ]
    for copy in loads[:4]:
        copy.start()

    barrier = pltpu.get_barrier_semaphore()

    def signal_sp(sem, d):
        for ok, to in ((sp >= d, sp - d), (sp + d < n_sp, sp + d)):

            @pl.when(ok)
            def _(to=to):
                pl.semaphore_signal(
                    sem, inc=1, device_id={"sp": to}, device_id_type=pl.DeviceIdType.MESH
                )

    def around(d):
        return jnp.where(sp >= d, 1, 0) + jnp.where(sp + d < n_sp, 1, 0)

    signal_sp(barrier, 1)
    for k in range(1, n_tp):
        pl.semaphore_signal(
            barrier, inc=1, device_id={"tp": lax.rem(tp + k, n_tp)},
            device_id_type=pl.DeviceIdType.MESH,
        )
    for copy in loads[4:10]:
        copy.start()
    for copy in loads[:4]:
        copy.wait()

    xf = tok[...].astype(F32)
    scale = lax.rsqrt(jnp.sum(xf * xf, axis=1, keepdims=True) / d_model + NORM_EPS)
    normed = (xf * scale * nin[...]).astype(BF16)
    for j in range(n_tp):
        for blk in range(n_blk):
            at = j * width + blk * LANES
            nsend[j, blk] = normed[:, at : at + LANES]

    side = LANES // state
    for i in range(width // group // side):
        cut = slice(i * LANES, (i + 1) * LANES)
        for src, dst in ((dlog, rows_a), (phase, rows_p)):
            row = jnp.concatenate([src[i * side + k : i * side + k + 1, :] for k in range(side)], axis=1)
            dst[:, cut] = jnp.broadcast_to(row, (8, LANES))

    for blk in range(n_blk):
        cut = slice(blk * lanes, (blk + 1) * lanes)
        a, p = rows_a[:, cut], rows_p[:, cut]
        k = lax.broadcasted_iota(jnp.int32, a.shape, 0).astype(F32)
        mag, cos, sin = jnp.exp(a), jnp.cos(p), jnp.sin(p)
        lr, li = mag * cos, mag * sin
        inv = jnp.exp(-a)
        nr, ni = inv * cos, -inv * sin
        mod = a * a + p * p
        cr = ((lr - 1.0) * a + li * p) / mod
        ci = (li * a - (lr - 1.0) * p) / mod
        one, zero = jnp.ones_like(a), jnp.zeros_like(a)
        pr, pi, mr, mi = one, zero, cr, ci
        sr, si, qr, qi = lr, li, nr, ni
        row = lax.broadcasted_iota(jnp.int32, a.shape, 0)
        for bit in range(3):
            on = lax.rem(row // (1 << bit), 2) == 1
            ar, ai = cmul(pr, pi, sr, si)
            pr, pi = jnp.where(on, ar, pr), jnp.where(on, ai, pi)
            ar, ai = cmul(mr, mi, qr, qi)
            mr, mi = jnp.where(on, ar, mr), jnp.where(on, ai, mi)
            sr, si = cmul(sr, si, sr, si)
            qr, qi = cmul(qr, qi, qr, qi)
        t2r[0:8, cut], t2i[0:8, cut], t1r[0:8, cut], t1i[0:8, cut] = pr, pi, mr, mi
        done = 8
        while done < rows:
            more = min(done, rows - done)
            for off in range(0, more, 8):
                src, dst = slice(off, off + 8), slice(done + off, done + off + 8)
                t2r[dst, cut], t2i[dst, cut] = cmul(t2r[src, cut], t2i[src, cut], sr, si)
                t1r[dst, cut], t1i[dst, cut] = cmul(t1r[src, cut], t1i[src, cut], qr, qi)
            sr, si = cmul(sr, si, sr, si)
            qr, qi = cmul(qr, qi, qr, qi)
            done += more
        lastr, lasti = t2r[rows - 1 : rows, cut], t2i[rows - 1 : rows, cut]
        wr, wi = cmul(lastr, lasti, lr[0:1], li[0:1])
        l_ref[blk : blk + 1, :] = wr
        l_ref[n_blk + blk : n_blk + blk + 1, :] = wi
        l_ref[2 * n_blk + blk : 2 * n_blk + blk + 1, :] = lr[0:1]
        l_ref[3 * n_blk + blk : 3 * n_blk + blk + 1, :] = li[0:1]

    pl.semaphore_wait(barrier, n_tp - 1 + around(1))

    sends = []
    for blk in range(n_blk):
        for k in range(1, n_tp):
            j = lax.rem(tp + n_tp - k, n_tp)
            copy = remote(
                nsend.at[j, blk], urecv.at[tp, blk], a_send.at[k, blk], a_recv.at[tp, blk], {"tp": j}
            )
            copy.start()
            sends.append(copy)
    if n_sp > 2:
        signal_sp(met.at[0], 1)
    for copy in loads[10:]:
        copy.start()
    urecv[tp] = nsend[tp]

    for copy in loads[4:10]:
        copy.wait()
    keep_c = (
        lax.broadcasted_iota(jnp.int32, (LANES, lanes), 0) // group
        == lax.broadcasted_iota(jnp.int32, (LANES, lanes), 1) // state
    )
    for blk in range(n_blk):
        for part, in_ref, out_ref in ((0, bre, cre), (1, bim, cim)):
            at = slice(part * lanes, (part + 1) * lanes)
            ch = slice(blk * LANES, (blk + 1) * LANES)
            b, c = in_ref[ch, :], out_ref[ch, :]
            wide = jnp.where(keep_c, jnp.concatenate([b] * per, axis=1), 0.0)
            bs[blk, :, at] = wide.astype(BF16)
            wide = jnp.where(keep_c, jnp.concatenate([c if part == 0 else -c] * per, axis=1), 0.0)
            cs[blk, :, at] = wide.astype(BF16)
    lower = (
        lax.broadcasted_iota(jnp.int32, (rows, rows), 0)
        >= lax.broadcasted_iota(jnp.int32, (rows, rows), 1)
    ).astype(BF16)

    d = 1
    hops = []
    while d < n_sp - 1:
        hops.append(d)
        d *= 2
    for r, d in enumerate(hops):
        if r > 0:
            signal_sp(met.at[r], d)
        if r < len(hops) - 1:
            pl.semaphore_wait(met.at[r], around(d))

    def end_copy(j, blk):
        return remote(
            e_send.at[blk], e_all.at[sp, blk], e_ssem.at[j, blk], e_rsem.at[sp, blk], {"sp": j}
        )

    for blk in range(n_blk):
        cut = slice(blk * lanes, (blk + 1) * lanes)
        ch = slice(blk * LANES, (blk + 1) * LANES)
        for k in range(1, n_tp):
            j = lax.rem(tp + k, n_tp)
            remote(
                nsend.at[j, blk], urecv.at[j, blk], a_send.at[k, blk], a_recv.at[j, blk], {"tp": j}
            ).wait_recv()
        for j in range(n_tp):
            uf[j * mine : (j + 1) * mine, ch] = urecv[j, blk].astype(F32)
        u = uf[:, ch].astype(BF16)
        d = jnp.dot(u, bs[blk], preferred_element_type=F32)
        wr, wi = cmul(d[:, :lanes], d[:, lanes:], t1r[:, cut], t1i[:, cut])
        wbuf[blk, :, :lanes] = wr.astype(BF16)
        wbuf[blk, :, lanes:] = wi.astype(BF16)
        er, ei = cmul(
            jnp.sum(wr, axis=0, keepdims=True), jnp.sum(wi, axis=0, keepdims=True),
            t2r[rows - 1 : rows, cut], t2i[rows - 1 : rows, cut],
        )
        e_send[blk] = jnp.concatenate([er, ei], axis=0).astype(BF16)

        if blk == 0 and hops:
            pl.semaphore_wait(met.at[len(hops) - 1], around(hops[-1]))

        def send_end(k, c, blk=blk):
            end_copy(n_sp - 1 - k, blk).start()
            return c

        lax.fori_loop(0, n_sp - 1 - sp, send_end, 0)

    for blk in range(n_blk):
        cut = slice(blk * lanes, (blk + 1) * lanes)
        s = jnp.dot(lower, wbuf[blk], preferred_element_type=F32)
        xr, xi = cmul(s[:, :lanes], s[:, lanes:], t2r[:, cut], t2i[:, cut])
        wbuf[blk, :, :lanes] = xr.astype(BF16)
        wbuf[blk, :, lanes:] = xi.astype(BF16)
        y = lax.dot_general(wbuf[blk], cs[blk], NT, preferred_element_type=F32)
        ch = slice(blk * LANES, (blk + 1) * LANES)
        ylocal[:, ch] = y + skip[:, ch] * uf[:, ch]

    for blk in range(n_blk):
        cut = slice(blk * lanes, (blk + 1) * lanes)
        ch = slice(blk * LANES, (blk + 1) * LANES)
        lr, li = l_ref[blk : blk + 1, :], l_ref[n_blk + blk : n_blk + blk + 1, :]

        def join(j, held, blk=blk, lr=lr, li=li):
            remote(
                e_send.at[blk], e_all.at[j, blk], e_ssem.at[j, blk], e_rsem.at[j, blk], {"sp": j}
            ).wait_recv()
            e = e_all[j, blk].astype(F32)
            hr, hi = cmul(*held, lr, li)
            return hr + e[0:1], hi + e[1:2]

        nil = jnp.zeros((1, lanes), F32)
        hr, hi = lax.fori_loop(0, sp, join, (nil, nil))
        hr, hi = cmul(
            hr, hi, l_ref[2 * n_blk + blk : 2 * n_blk + blk + 1, :], l_ref[3 * n_blk + blk : 3 * n_blk + blk + 1, :]
        )
        xr, xi = cmul(hr, hi, t2r[:, cut], t2i[:, cut])
        wbuf[blk, :, :lanes] = xr.astype(BF16)
        wbuf[blk, :, lanes:] = xi.astype(BF16)
        y = lax.dot_general(wbuf[blk], cs[blk], NT, preferred_element_type=F32)
        zbuf[tp, blk] = jax.nn.gelu(y + ylocal[:, ch]).astype(BF16)
        for k in range(1, n_chip):
            j = lax.rem(tp + 2 * k, n_tp)
            copy = remote(
                zbuf.at[tp, blk], zbuf.at[tp, blk], z_send.at[k, blk], z_recv.at[tp, blk], {"tp": j}
            )
            copy.start()
            sends.append(copy)
        copy = remote(
            zbuf.at[tp, blk], zbuf.at[tp, blk], z_send.at[0, blk], z_recv.at[tp, blk], {"tp": partner}
        )
        copy.start()
        sends.append(copy)

    for copy in loads[10:]:
        copy.wait()

    def arrived(j, blk):
        remote(
            zbuf.at[j, blk], zbuf.at[j, blk], z_send.at[0, blk], z_recv.at[j, blk], {"tp": partner}
        ).wait_recv()

    def project(j, blk, first=False):
        at = pl.ds(pl.multiple_of(j * width + blk * LANES, LANES), LANES)
        z = zbuf[j, blk]
        v = jnp.dot(z, wv[at, :], preferred_element_type=F32)
        g = jnp.dot(z, wg[at, :], preferred_element_type=F32)
        if first:
            acc_v[...], acc_g[...] = v, g
        else:
            acc_v[...] += v
            acc_g[...] += g

    for blk in range(n_blk):
        project(tp, blk, blk == 0)
    for blk in range(n_blk):
        arrived(partner, blk)
        project(partner, blk)
    late = []
    for blk in range(n_blk):
        for k in range(1, n_chip):
            j = lax.rem(tp + n_tp - 2 * k, n_tp)
            arrived(j, blk)
            copy = remote(
                zbuf.at[j, blk], zbuf.at[j, blk], f_send.at[k, blk], z_recv.at[j, blk], {"tp": partner}
            )
            copy.start()
            sends.append(copy)
            project(j, blk)
            late.append((lax.rem(partner + n_tp - 2 * k, n_tp), blk))
            if len(late) > 1:
                item = late.pop(0)
                arrived(*item)
                project(*item)
    for item in late:
        arrived(*item)
        project(*item)

    gated = acc_v[...] * jax.nn.sigmoid(acc_g[...])
    acc_v[...] = gated
    square = gated * gated
    part = square[:, :LANES]
    for blk in range(1, n_blk):
        part = part + square[:, blk * LANES : (blk + 1) * LANES]
    total = exact(jnp.ones((8, LANES), BF16), part)
    sq_all[tp] = total[0:1]
    for k in range(1, n_tp):
        j = lax.rem(tp + n_tp - k, n_tp)
        copy = remote(sq_all.at[tp], sq_all.at[tp], q_send.at[k], q_recv.at[tp], {"tp": j})
        copy.start()
        sends.append(copy)
    total = total[0:1]
    for k in range(1, n_tp):
        j = lax.rem(tp + k, n_tp)
        remote(sq_all.at[j], sq_all.at[j], q_send.at[k], q_recv.at[j], {"tp": j}).wait_recv()
        total = total + sq_all[j]
    scale = lax.rsqrt(total / d_model + NORM_EPS)
    eye = (
        lax.broadcasted_iota(jnp.int32, (rows, rows), 0)
        == lax.broadcasted_iota(jnp.int32, (rows, rows), 1)
    ).astype(BF16)
    column = exact(eye, jnp.broadcast_to(scale, (LANES, rows)))
    for blk in range(n_blk):
        ch = slice(blk * LANES, (blk + 1) * LANES)
        out[:, ch] = (acc_v[:, ch] * column * nout[:, ch]).astype(BF16)

    for copy in sends:
        copy.wait_send()

    def sent(j, c):
        for blk in range(n_blk):
            end_copy(j, blk).wait_send()
        return c

    lax.fori_loop(sp + 1, n_sp, sent, 0)


def solution(mesh):
    n_sp, n_tp = mesh.shape["sp"], mesh.shape["tp"]

    def on_device(
        tokens, norm_in, decay_log, phase, b_real, b_imag, c_real, c_imag, skip_gain, w_value, w_gate, norm_out
    ):
        mine, d_model = tokens.shape
        rows = mine * n_tp
        groups, state, group = b_real.shape
        width = groups * group
        n_blk = width // LANES
        lanes = LANES // group * state
        entries = groups * state
        vmem = pl.BlockSpec(memory_space=pltpu.VMEM)
        hbm = pl.BlockSpec(memory_space=pl.ANY)
        dma = pltpu.SemaphoreType.DMA
        return pl.pallas_call(
            functools.partial(layer, n_sp, n_tp, state, group),
            out_shape=pltpu.VMEM((rows, width), BF16),
            in_specs=[hbm] * 12,
            out_specs=vmem,
            scratch_shapes=[
                pltpu.VMEM((n_tp, n_blk, mine, LANES), BF16),
                pltpu.VMEM((n_tp, n_blk, mine, LANES), BF16),
                pltpu.VMEM((rows, width), F32),
                pltpu.VMEM((8, entries), F32),
                pltpu.VMEM((8, entries), F32),
                pltpu.VMEM((rows, entries), F32),
                pltpu.VMEM((rows, entries), F32),
                pltpu.VMEM((rows, entries), F32),
                pltpu.VMEM((rows, entries), F32),
                pltpu.VMEM((n_blk, LANES, 2 * lanes), BF16),
                pltpu.VMEM((n_blk, LANES, 2 * lanes), BF16),
                pltpu.VMEM((n_blk, rows, 2 * lanes), BF16),
                pltpu.VMEM((rows, width), F32),
                pltpu.VMEM((n_blk, 2, lanes), BF16),
                pltpu.VMEM((n_sp, n_blk, 2, lanes), BF16),
                pltpu.VMEM((4 * n_blk, lanes), F32),
                pltpu.VMEM((n_tp, n_blk, rows, LANES), BF16),
                pltpu.VMEM(w_value.shape, BF16),
                pltpu.VMEM(w_gate.shape, BF16),
                pltpu.VMEM((rows, width), F32),
                pltpu.VMEM((rows, width), F32),
                pltpu.VMEM((n_tp, 1, rows), F32),
                pltpu.VMEM((width, state), F32),
                pltpu.VMEM((width, state), F32),
                pltpu.VMEM((width, state), F32),
                pltpu.VMEM((width, state), F32),
                pltpu.VMEM((mine, d_model), BF16),
                pltpu.VMEM((1, d_model), F32),
                pltpu.VMEM((groups, state), F32),
                pltpu.VMEM((groups, state), F32),
                pltpu.VMEM((1, width), F32),
                pltpu.VMEM((1, width), F32),
                dma((12,)),
                dma((n_tp, n_blk)),
                dma((n_tp, n_blk)),
                dma((n_sp, n_blk)),
                dma((n_sp, n_blk)),
                dma((n_tp // 2, n_blk)),
                dma((n_tp, n_blk)),
                dma((n_tp // 2, n_blk)),
                dma((n_tp,)),
                dma((n_tp,)),
                pltpu.SemaphoreType.REGULAR((max(n_sp.bit_length(), 1),)),
            ],
            compiler_params=pltpu.CompilerParams(collective_id=0, has_side_effects=True),
        )(
            tokens,
            norm_in.reshape(1, -1),
            decay_log,
            phase,
            b_real.transpose(0, 2, 1).reshape(width, state),
            b_imag.transpose(0, 2, 1).reshape(width, state),
            c_real.reshape(width, state),
            c_imag.reshape(width, state),
            skip_gain.reshape(1, -1),
            w_value,
            w_gate,
            norm_out.reshape(1, -1),
        )

    placed = (
        P(("sp", "tp"), None),
        P(),
        P("tp", None),
        P("tp", None),
        P("tp", None, None),
        P("tp", None, None),
        P("tp", None, None),
        P("tp", None, None),
        P("tp"),
        P(None, "tp"),
        P(None, "tp"),
        P("tp"),
    )
    return jax.shard_map(
        on_device, mesh=mesh, in_specs=placed, out_specs=P("sp", "tp"), check_vma=False
    )
```
